32 devices in a mesh: kv: 16 (over z, y, x), tp: 2 (over core).
Axes of the slice: x: 2, y: 2, z: 4, core: 2. Of those that a mesh axis runs over, the one named last changes fastest.
Arguments:
- tokens: bfloat16 [160, 3, 2048], P('kv', None, 'tp'), may hold values from -6 to 6
- norm_gain: float32 [2048], replicated, may hold values from 0.1 to 1.9
- w_query: bfloat16 [2048, 1024], P('kv', 'tp'), may hold values from -0.125 to 0.125
- w_key: bfloat16 [2048, 1024], P('kv', 'tp'), may hold values from -0.125 to 0.125
- w_value: bfloat16 [2048, 2048], P('kv', 'tp'), may hold values from -0.125 to 0.125
- w_igate: bfloat16 [2048, 8], replicated, may hold values from -0.125 to 0.125
- w_fgate: bfloat16 [2048, 8], replicated, may hold values from -0.125 to 0.125
- igate_bias: float32 [8], replicated, may hold values from -5 to -2
- fgate_bias: float32 [8], replicated, may hold values from 0.5 to 4
- prev_keys: bfloat16 [160, 3, 1024], P('kv', None, 'tp'), may hold values from -6 to 6
- prev_values: bfloat16 [160, 3, 2048], P('kv', None, 'tp'), may hold values from -6 to 6
- prev_igate: float32 [160, 3, 8], P('kv', None, 'tp'), may hold values from -4 to 0
- prev_logf: float32 [160, 3, 8], P('kv', None, 'tp'), may hold values from -0.6 to -0.02
- accepted: int32 [160], P('kv'), may hold values from 0 to 3
- state_mem: float32 [160, 8, 128, 256], P('kv', 'tp'), may hold values from -2 to 2
- state_norm: float32 [160, 8, 128], P('kv', 'tp'), may hold values from -2 to 2
- state_max: float32 [160, 8], P('kv', 'tp'), may hold values from -3 to 0
Outputs:
- readout: bfloat16 [160, 3, 2048], P('kv', None, 'tp')
- base_mem: float32 [160, 8, 128, 256], P('kv', 'tp')
- base_norm: float32 [160, 8, 128], P('kv', 'tp')
- base_max: float32 [160, 8], P('kv', 'tp')
The draws below stay inside these ranges and needn't reach their ends.
Inputs may be any that keep to these rules, and one draw needn't show every extreme that they name: Proposal j of a sequence is live when j < accepted of that sequence.
All inputs are finite; a program needn't handle non-finite values.
Results may differ from the reference program's by a relative error of at most 0.0073.
Values may be sent and summed in bfloat16 or wider, within the bound.
No kernel may reach another device: no remote copies, remote signals or barrier semaphores. Data moves between devices by JAX's collectives and lax.ppermute only.
A program may use at most 64 MiB of HBM per device.

```python
import jax
import jax.numpy as jnp
from jax import lax

D = 2048
HEADS = 8
DK = 128
DV = 256
PROPOSALS = 3
SEQS = 160


def draw_state_max(key, part):
    first = jax.random.fold_in(key, 0)
    settled = jax.random.uniform(first, (SEQS, HEADS), jnp.float32, -3.0, 0.0)
    return settled


def set_ends(values, rng, low, top_value):
    place = [jax.random.randint(jax.random.fold_in(rng, axis), (), 0, length) for axis, length in enumerate(values.shape)]
    longest = values.shape.index(max(values.shape))
    beside = place[:longest] + [(place[longest] + 1) % values.shape[longest]] + place[longest + 1:]
    return values.at[tuple(place)].set(low).at[tuple(beside)].set(top_value)


def block_levels(rng, shape, shards, least, largest):
    level, own = 1.0, jax.random.fold_in(rng, 6)
    for position, shards_of in shards:
        steps = jnp.exp(jax.random.uniform(jax.random.fold_in(own, position), (shards_of,), jnp.float32, least / len(shards), largest / len(shards)))
        level = level * jnp.repeat(steps, shape[position] // shards_of).reshape([-1 if axis == position else 1 for axis in range(len(shape))])
    return level


def gaussian(own_key, extent, spread, bound, pieces=(), held_as=jnp.bfloat16):
    values = jax.random.normal(own_key, extent, jnp.float32) * spread
    if len(pieces) > 0:
        values = block_levels(own_key, extent, pieces, -0.22, 0.18) * values
    return jnp.clip(values, min=-bound, max=bound).astype(held_as)


def setup_inputs(seed: int = 0) -> dict:
    arg_keys = jax.random.split(jax.random.key(seed), 18)
    return {
        "tokens": gaussian(arg_keys[0], (SEQS, PROPOSALS, D), 1.0, 6.0, ((0, 16), (2, 2))),
        "norm_gain": jnp.clip(1.0 + 0.18 * jax.random.normal(arg_keys[1], (D,), jnp.float32), 0.1, 1.9),
        "w_query": gaussian(arg_keys[2], (D, HEADS * DK), D ** -0.5, 0.125, ((0, 16), (1, 2))),
        "w_key": gaussian(arg_keys[3], (D, HEADS * DK), D ** -0.5, 0.125, ((0, 16), (1, 2))),
        "w_value": gaussian(arg_keys[4], (D, HEADS * DV), D ** -0.5, 0.125, ((0, 16), (1, 2))),
        "w_igate": gaussian(arg_keys[5], (D, HEADS), D ** -0.5, 0.125),
        "w_fgate": gaussian(arg_keys[6], (D, HEADS), D ** -0.5, 0.125),
        "igate_bias": jnp.clip(jax.random.uniform(arg_keys[7], (HEADS,), jnp.float32, -5.0, -2.0), -5.0, -2.0),
        "fgate_bias": jnp.clip(jax.random.uniform(arg_keys[8], (HEADS,), jnp.float32, 0.5, 4.0), 0.5, 4.0),
        "prev_keys": gaussian(arg_keys[9], (SEQS, PROPOSALS, HEADS * DK), 1.0, 6.0, ((0, 16), (2, 2))),
        "prev_values": gaussian(arg_keys[10], (SEQS, PROPOSALS, HEADS * DV), 1.0, 6.0, ((0, 16), (2, 2))),
        "prev_igate": jnp.clip(-4.0 + 4.0 * jax.random.uniform(arg_keys[11], (SEQS, PROPOSALS, HEADS), jnp.float32) ** block_levels(arg_keys[11], (SEQS, PROPOSALS, HEADS), ((0, 16), (2, 2)), -0.2, 0.2), -4.0, 0.0),
        "prev_logf": jnp.clip(-0.6 + 0.58000002 * jax.random.uniform(arg_keys[12], (SEQS, PROPOSALS, HEADS), jnp.float32) ** block_levels(arg_keys[12], (SEQS, PROPOSALS, HEADS), ((0, 16), (2, 2)), -0.2, 0.2), -0.6, -0.02),
        "accepted": set_ends(jax.random.randint(arg_keys[13], (SEQS,), 0, PROPOSALS + 1), jax.random.fold_in(arg_keys[13], 1), 0, PROPOSALS).astype(jnp.int32),
        "state_mem": gaussian(arg_keys[14], (SEQS, HEADS, DK, DV), 0.3, 2.0, ((0, 16), (1, 2)), jnp.float32),
        "state_norm": gaussian(arg_keys[15], (SEQS, HEADS, DK), 0.3, 2.0, ((0, 16), (1, 2)), jnp.float32),
        "state_max": draw_state_max(jax.random.fold_in(arg_keys[17], 71), 0),
    }


epsilon = 1e-06
highest = lax.Precision.HIGHEST

def fold_accepted(state_mem, state_norm, state_max, key_rows, value_rows, in_gate, log_forget, accepted):
    length = key_rows.shape[1]
    live_mask = (jnp.arange(length, dtype=jnp.int32)[None, :] < accepted[:, None])[:, :, None]
    forget_live = jnp.where(live_mask, log_forget, 0.0)
    cumulative = jnp.cumsum(forget_live, axis=1)
    totals = cumulative[:, -1]
    weight_log = jnp.where(live_mask, totals[:, None] - cumulative + in_gate, -jnp.inf)
    base_max = jnp.maximum(totals + state_max, lax.optimization_barrier(jnp.max(weight_log, axis=1)))
    carry_weight = jnp.exp(totals + state_max - base_max)
    weights = jnp.exp(weight_log - base_max[:, None])
    base_mem = carry_weight[..., None, None] * state_mem + jnp.einsum('sph,sphd,sphv->shdv', weights, key_rows, value_rows, precision=highest)
    base_norm = carry_weight[..., None] * state_norm + jnp.einsum('sph,sphd->shd', weights, key_rows, precision=highest)
    return (base_mem, base_norm, base_max)

def readout_block(base_mem, base_norm, base_max, query_rows, key_rows, value_rows, in_gate, log_forget):
    length = query_rows.shape[1]
    cumulative = jnp.cumsum(log_forget, axis=1)
    causal = jnp.arange(length, dtype=jnp.int32)[:, None] >= jnp.arange(length, dtype=jnp.int32)[None, :]
    within_log = cumulative[:, :, None, :] - cumulative[:, None, :, :] + in_gate[:, None, :, :]
    within_log = jnp.where(causal[None, :, :, None], within_log, -jnp.inf)
    carried_log = cumulative + base_max[:, None, :]
    top_log = jnp.maximum(carried_log, lax.optimization_barrier(jnp.max(within_log, axis=2)))
    scores = jnp.einsum('sthd,suhd->stuh', query_rows, key_rows, precision=highest) * jnp.exp(within_log - top_log[:, :, None, :])
    carried_weight = jnp.exp(carried_log - top_log)
    numerator = jnp.einsum('stuh,suhv->sthv', scores, value_rows, precision=highest) + carried_weight[..., None] * jnp.einsum('sthd,shdv->sthv', query_rows, base_mem, precision=highest)
    denominator = lax.optimization_barrier(jnp.sum(scores, axis=2)) + carried_weight * jnp.einsum('sthd,shd->sth', query_rows, base_norm, precision=highest)
    return numerator / jnp.maximum(jnp.abs(denominator), jnp.exp(-top_log))[..., None]

def reference(tokens, norm_gain, w_query, w_key, w_value, w_igate, w_fgate, igate_bias, fgate_bias, prev_keys, prev_values, prev_igate, prev_logf, accepted, state_mem, state_norm, state_max):
    seq_count, length, model_width = tokens.shape
    head_count = igate_bias.shape[0]
    key_width = state_mem.shape[2]
    value_width = state_mem.shape[3]
    key_scale = key_width ** (-0.5)
    flattened = tokens.reshape(seq_count * length, model_width).astype(jnp.float32)
    normed = (flattened * lax.rsqrt(lax.optimization_barrier(jnp.mean(flattened * flattened, axis=-1, keepdims=True)) + epsilon) * norm_gain).astype(jnp.bfloat16)
    query_rows = jnp.dot(normed, w_query, preferred_element_type=jnp.float32).astype(jnp.bfloat16)
    key_rows = jnp.dot(normed, w_key, preferred_element_type=jnp.float32).astype(jnp.bfloat16)
    value_rows = jnp.dot(normed, w_value, preferred_element_type=jnp.float32).astype(jnp.bfloat16)
    in_gate = jnp.dot(normed, w_igate, preferred_element_type=jnp.float32) + igate_bias
    log_forget = jax.nn.log_sigmoid(jnp.dot(normed, w_fgate, preferred_element_type=jnp.float32) + fgate_bias)

    def split_heads(matrix, last_width):
        return matrix.astype(jnp.float32).reshape(seq_count, length, head_count, last_width)
    base_mem, base_norm, base_max = fold_accepted(state_mem, state_norm, state_max, split_heads(prev_keys, key_width) * key_scale, split_heads(prev_values, value_width), prev_igate, prev_logf, accepted)
    hidden = readout_block(base_mem, base_norm, base_max, split_heads(query_rows, key_width), split_heads(key_rows, key_width) * key_scale, split_heads(value_rows, value_width), in_gate.reshape(seq_count, length, head_count), log_forget.reshape(seq_count, length, head_count))
    readout = hidden.reshape(seq_count, length, head_count * value_width).astype(jnp.bfloat16)
    return (readout, base_mem, base_norm, base_max)
```

```python
import jax
import jax.numpy as jnp
from jax import lax
from jax.experimental import pallas as pl
from jax.experimental.pallas import tpu as pltpu
from jax.sharding import PartitionSpec as P

epsilon = 1e-06
highest = lax.Precision.HIGHEST


def stack_columns(parts):
    widths = [part.shape[1] for part in parts]

    def body(*refs):
        sources, target, arrived = refs[: len(parts)], refs[len(parts)], refs[len(parts) + 1]
        copies, start = [], 0
        for index, width in enumerate(widths):
            copies.append(
                pltpu.make_async_copy(
                    sources[index], target.at[:, start : start + width], arrived.at[index]
                )
            )
            start += width
        for copy in copies:
            copy.start()
        for copy in copies:
            copy.wait()

    return pl.pallas_call(
        body,
        in_specs=[pl.BlockSpec(memory_space=pl.ANY)] * len(parts),
        out_specs=pl.BlockSpec(memory_space=pltpu.VMEM),
        out_shape=jax.ShapeDtypeStruct((parts[0].shape[0], sum(widths)), parts[0].dtype),
        scratch_shapes=[pltpu.SemaphoreType.DMA((len(parts),))],
    )(*parts)


def split_terms(value):
    high = value.astype(jnp.bfloat16).astype(jnp.float32)
    middle = (value - high).astype(jnp.bfloat16).astype(jnp.float32)
    return [high, middle, value - high - middle]


def fold_body(
    accepted_ref,
    keys_ref,
    values_ref,
    gate_ref,
    mem_ref,
    norm_ref,
    mem_out,
    norm_out,
    max_out,
):
    seq = pl.program_id(0)
    count = accepted_ref[seq]
    length = keys_ref.shape[1]
    _, head_count, key_width, value_width = mem_ref.shape
    key_scale = key_width ** (-0.5)
    gates = gate_ref[seq]
    forgets = gates[length : 2 * length]
    total = jnp.zeros((1, head_count), jnp.float32)
    cumulative = []
    for j in range(length):
        total = total + jnp.where(j < count, forgets[j : j + 1], 0.0)
        cumulative.append(total)
    carried = total + gates[2 * length : 2 * length + 1]
    logs = [
        jnp.where(j < count, total - cumulative[j] + gates[j : j + 1], -jnp.inf)
        for j in range(length)
    ]
    top = carried
    for log in logs:
        top = jnp.maximum(top, log)
    max_out[pl.ds(seq, 1), :] = top
    carry = jnp.exp(carried - top)
    weights = jnp.concatenate([jnp.exp(log - top) for log in logs], axis=0)
    keys = keys_ref[seq].astype(jnp.float32) * key_scale
    values = values_ref[seq].astype(jnp.float32)
    fill = -3 * length % 16
    for head in range(head_count):
        head_carry = carry[:, head : head + 1]
        weighted = (
            weights[:, head : head + 1] * keys[:, head * key_width : (head + 1) * key_width]
        )
        norm_out[seq, head : head + 1, :] = head_carry * norm_ref[
            seq, head : head + 1, :
        ] + jnp.sum(weighted, axis=0, keepdims=True)
        left = jnp.concatenate(
            split_terms(weighted) + [jnp.zeros((fill, key_width), jnp.float32)], axis=0
        ).astype(jnp.bfloat16)
        head_values = values[:, head * value_width : (head + 1) * value_width]
        right = jnp.concatenate(
            [head_values] * 3 + [jnp.zeros((fill, value_width), jnp.float32)], axis=0
        ).astype(jnp.bfloat16)
        update = lax.dot_general(
            left, right, (((0,), (0,)), ((), ())), preferred_element_type=jnp.float32
        )
        mem_out[0, head] = head_carry * mem_ref[0, head] + update


def fold_accepted(
    state_mem, state_norm, state_max, prev_keys, prev_values, in_gate, log_forget, accepted
):
    block = pl.BlockSpec((1,) + state_mem.shape[1:], lambda seq: (seq, 0, 0, 0))

    length = in_gate.shape[1]
    packed = (
        jnp.pad(in_gate, ((0, 0), (0, length + 1), (0, 0)))
        + jnp.pad(log_forget, ((0, 0), (length, 1), (0, 0)))
        + jnp.pad(state_max[:, None], ((0, 0), (2 * length, 0), (0, 0)))
    )

    def whole(array):
        rank = array.ndim
        return pl.BlockSpec(array.shape, lambda seq: (0,) * rank)

    return pl.pallas_call(
        fold_body,
        grid=(state_mem.shape[0],),
        in_specs=[
            pl.BlockSpec(memory_space=pltpu.SMEM),
            whole(prev_keys),
            whole(prev_values),
            whole(packed),
            block,
            whole(state_norm),
        ],
        out_specs=[block, whole(state_norm), whole(state_max)],
        out_shape=[
            jax.ShapeDtypeStruct(state_mem.shape, jnp.float32),
            jax.ShapeDtypeStruct(state_norm.shape, jnp.float32),
            jax.ShapeDtypeStruct(state_max.shape, jnp.float32),
        ],
    )(accepted, prev_keys, prev_values, packed, state_mem, state_norm)


def readout_block(
    base_mem, base_norm, base_max, query_rows, key_rows, value_rows, in_gate, log_forget
):
    length = query_rows.shape[1]
    causal = (
        jnp.arange(length, dtype=jnp.int32)[:, None] >= jnp.arange(length, dtype=jnp.int32)[None, :]
    )
    cumulative = jnp.sum(jnp.where(causal[None, :, :, None], log_forget[:, None], 0.0), axis=2)
    within_log = cumulative[:, :, None, :] - cumulative[:, None, :, :] + in_gate[:, None, :, :]
    within_log = jnp.where(causal[None, :, :, None], within_log, -jnp.inf)
    carried_log = cumulative + base_max[:, None, :]
    top_log = jnp.maximum(carried_log, jnp.max(within_log, axis=2))
    scores = jnp.einsum("sthd,suhd->stuh", query_rows, key_rows, precision=highest) * jnp.exp(
        within_log - top_log[:, :, None, :]
    )
    carried_weight = jnp.exp(carried_log - top_log)
    numerator = jnp.einsum(
        "stuh,suhv->sthv", scores, value_rows, precision=highest
    ) + carried_weight[..., None] * jnp.einsum(
        "sthd,shdv->sthv", query_rows, base_mem, precision=lax.Precision.DEFAULT
    )
    denominator = jnp.sum(scores, axis=2) + carried_weight * jnp.einsum(
        "sthd,shd->sth", query_rows, base_norm, precision=highest
    )
    return numerator / jnp.maximum(jnp.abs(denominator), jnp.exp(-top_log))[..., None]


def group_shift(outer, inner, order, step, along_inner):
    size = len(order)
    pairs = []
    for other in range(outer if along_inner else inner):
        for place in range(size):
            source, target = order[place], order[(place + step) % size]
            if along_inner:
                pairs.append((other * inner + source, other * inner + target))
            else:
                pairs.append((source * inner + other, target * inner + other))
    return pairs


def ring_gather(block, outer, inner, order):
    def forward(part):
        return lax.ppermute(part, "kv", group_shift(outer, inner, order, 1, True))

    def backward(part):
        return lax.ppermute(part, "kv", group_shift(outer, inner, order, -1, True))

    found = [(0, block)]
    ahead = behind = block
    for distance in range(1, (inner + 1) // 2):
        ahead, behind = forward(ahead), backward(behind)
        found += [(distance, ahead), (-distance, behind)]
    if inner % 2 == 0:
        half = block.shape[0] // 2
        far = jnp.concatenate([forward(ahead[:half]), backward(behind[half:])], axis=0)
        found.append((inner // 2, far))
    return found


def shards(
    tokens,
    norm_gain,
    w_query,
    w_key,
    w_value,
    w_igate,
    w_fgate,
    igate_bias,
    fgate_bias,
    prev_keys,
    prev_values,
    prev_igate,
    prev_logf,
    accepted,
    state_mem,
    state_norm,
    state_max,
):
    seq_count, length, part_width = tokens.shape
    head_count = state_mem.shape[1]
    key_width = state_mem.shape[2]
    value_width = state_mem.shape[3]
    key_scale = key_width ** (-0.5)
    row_count = seq_count * length
    gathered = lax.all_gather(tokens.reshape(row_count, part_width), "tp", axis=1, tiled=True)
    flattened = gathered.astype(jnp.float32)
    normed = (
        flattened
        * lax.rsqrt(jnp.mean(flattened * flattened, axis=-1, keepdims=True) + epsilon)
        * norm_gain
    ).astype(jnp.bfloat16)
    kv_count = lax.axis_size("kv")
    inner = 1 << ((kv_count.bit_length() - 1) // 2)
    outer = kv_count // inner
    order = [place ^ (place >> 1) for place in range(inner)]
    outer_order = list(range(outer))
    rank = lax.axis_index("kv")
    outer_rank, inner_rank = rank // inner, rank % inner
    ring_place = inner_rank ^ (inner_rank >> 1)
    for shift in range(2, inner.bit_length()):
        ring_place = ring_place ^ (inner_rank >> shift)
    block_rows = -(-row_count // 16) * 16
    slice_width = w_query.shape[0]
    group_width = inner * slice_width

    weights = ring_gather(stack_columns([w_query, w_key, w_value]), outer, inner, order)

    normed_later, near = lax.optimization_barrier((normed, weights[1][1]))
    weights[1] = (weights[1][0], near)

    padded = jnp.pad(normed, ((0, block_rows - row_count), (0, 0)))
    blocks = []
    for step in range(outer):
        part = lax.dynamic_slice_in_dim(
            padded, ((outer_rank + step) % outer) * group_width, group_width, 1
        )
        if step:
            part = lax.ppermute(
                part, "kv", group_shift(outer, inner, outer_order, step, False)
            )
        blocks.append(part)
    spread = jnp.concatenate(blocks, axis=0)

    def project(pieces, accepted):
        total = None
        for distance, weight in pieces:
            place = (ring_place - distance) % inner
            source = place ^ (place >> 1)
            columns = lax.dynamic_slice_in_dim(spread, source * slice_width, slice_width, 1)
            product = jnp.dot(columns, weight, preferred_element_type=jnp.float32)
            total = product if total is None else total + product
        total, held = lax.optimization_barrier((total, accepted))
        own = total[:block_rows]
        for step in range(1, outer):
            partial = total[step * block_rows : (step + 1) * block_rows].astype(jnp.bfloat16)
            own = own + lax.ppermute(
                partial, "kv", group_shift(outer, inner, outer_order, -step, False)
            ).astype(jnp.float32)
        return own[:row_count].astype(jnp.bfloat16), held

    query_cols = head_count * key_width
    projected, accepted = project(weights, accepted)
    query_rows = projected[:, :query_cols]
    key_rows = projected[:, query_cols : 2 * query_cols]
    value_rows = projected[:, 2 * query_cols :]
    head_start = lax.axis_index("tp") * head_count
    input_weight = lax.dynamic_slice_in_dim(w_igate, head_start, head_count, 1)
    forget_weight = lax.dynamic_slice_in_dim(w_fgate, head_start, head_count, 1)
    in_gate = jnp.dot(
        normed_later, input_weight, preferred_element_type=jnp.float32
    ) + lax.dynamic_slice_in_dim(igate_bias, head_start, head_count, 0)
    log_forget = jax.nn.log_sigmoid(
        jnp.dot(normed_later, forget_weight, preferred_element_type=jnp.float32)
        + lax.dynamic_slice_in_dim(fgate_bias, head_start, head_count, 0)
    )

    def split_heads(matrix, last_width):
        return matrix.astype(jnp.float32).reshape(seq_count, length, head_count, last_width)

    base_mem, base_norm, base_max = fold_accepted(
        state_mem,
        state_norm,
        state_max,
        prev_keys,
        prev_values,
        prev_igate,
        prev_logf,
        accepted,
    )
    hidden = readout_block(
        base_mem,
        base_norm,
        base_max,
        split_heads(query_rows, key_width),
        split_heads(key_rows, key_width) * key_scale,
        split_heads(value_rows, value_width),
        in_gate.reshape(seq_count, length, head_count),
        log_forget.reshape(seq_count, length, head_count),
    )
    readout = hidden.reshape(seq_count, length, head_count * value_width).astype(jnp.bfloat16)
    return (readout, base_mem, base_norm, base_max)


def solution(mesh):
    return jax.shard_map(
        shards,
        mesh=mesh,
        in_specs=(
            P("kv", None, "tp"),
            P(),
            P("kv", "tp"),
            P("kv", "tp"),
            P("kv", "tp"),
            P(),
            P(),
            P(),
            P(),
            P("kv", None, "tp"),
            P("kv", None, "tp"),
            P("kv", None, "tp"),
            P("kv", None, "tp"),
            P("kv"),
            P("kv", "tp", None, None),
            P("kv", "tp", None),
            P("kv", "tp"),
        ),
        out_specs=(
            P("kv", None, "tp"),
            P("kv", "tp", None, None),
            P("kv", "tp", None),
            P("kv", "tp"),
        ),
        check_vma=False,
    )
```
